32 devices in a mesh: ep: 4 (over y, x), tp: 8 (over z, core).
Axes of the slice: x: 2, y: 2, z: 4, core: 2. Of those that a mesh axis runs over, the one named last changes fastest.
Arguments:
- tokens: bfloat16 [1024, 2048], P('ep'), may hold values from -6 to 6
- cotangent: bfloat16 [1024, 2048], P('ep'), may hold values from -6 to 6
- group_prob: float32 [1024], P('ep'), may hold values from 0.25 to 1
- expert_prob: float32 [1024, 2], P('ep'), may hold values from 0.1 to 1
- routing: int32 [1024, 2], P('ep'), may hold values from 0 to 3, all different within a row; in each aligned block of 256 rows (0 to 255, 256 to 511, ...) at most 192 rows name the same one
- gate_weight: bfloat16 [4, 2048, 4096], P('ep', None, 'tp'), may hold values from -0.125 to 0.125
- up_weight: bfloat16 [4, 2048, 4096], P('ep', None, 'tp'), may hold values from -0.125 to 0.125
- down_weight: bfloat16 [4, 4096, 2048], P('ep', 'tp'), may hold values from -1 to 1
Outputs:
- token_grad: bfloat16 [1024, 2048], P('ep')
- group_prob_grad: float32 [1024], P('ep')
- expert_prob_grad: float32 [1024, 2], P('ep')
- gate_weight_grad: bfloat16 [4, 2048, 4096], P('ep', None, 'tp')
- up_weight_grad: bfloat16 [4, 2048, 4096], P('ep', None, 'tp')
- down_weight_grad: bfloat16 [4, 4096, 2048], P('ep', 'tp')
- gate_row_norms: float32 [4, 2048], P('ep')
- up_row_norms: float32 [4, 2048], P('ep')
- down_row_norms: float32 [4, 4096], P('ep', 'tp')
The draws below stay inside these ranges and needn't reach their ends.
Inputs may be any that keep to these rules, and one draw needn't show every extreme that they name: `routing`: each row names 2 different experts. In each aligned block of 256 rows no expert is named by more than 192 rows, and in every draw some expert is named by exactly 192 rows of some block.
All inputs are finite; a program needn't handle non-finite values.
Results may differ from the reference program's by a relative error of at most 0.0065.
Values may be sent and summed in bfloat16 or wider, within the bound.
A program may use at most 64 MiB of HBM per device.

```python
import math
import jax
import jax.numpy as jnp
import numpy as np
from jax import lax

D = 2048
FF = 4096
TOP_K = 2
TOK_DEV = 256
EXPERTS = 4
CAP = 192
TOKENS = 1024
N_EP = 4


def draw_down_weight(key, part):
    first, second = jax.random.split(key, 2)
    base = jax.random.normal(first, (EXPERTS, FF, D), jnp.float32)
    rough = jax.random.uniform(second, (EXPERTS, FF, 1), jnp.float32, 0.0, 1.0)
    position = jnp.arange(FF, dtype=jnp.float32).reshape(1, FF, 1) / FF
    log_scale = jnp.log(10.0) * (rough - 0.5) + jnp.log(3.0) * (position - 0.5)
    scale = jnp.exp(log_scale)
    scale = scale / jnp.sqrt(jnp.mean(scale * scale, axis=1, keepdims=True))
    values = jnp.clip(base * scale * FF ** (-0.5), -1.0, 1.0)
    return values.astype(jnp.bfloat16)


def block_scale(rng, dims, cuts, smallest, largest):
    factor_of = 1.0
    for axis_at, parts in cuts:
        steps = jax.random.uniform(jax.random.fold_in(jax.random.fold_in(rng, 6), axis_at), (parts,), jnp.float32, smallest / len(cuts), largest / len(cuts))
        factor_of = factor_of * jnp.repeat(jnp.exp(steps), dims[axis_at] // parts).reshape((-1,) + (1,) * (len(dims) - 1 - axis_at))
    return factor_of


def assign_block(rng, own, number, rows, amount, top, bound, skew):
    ranking = jax.random.permutation(rng, amount)
    heavy_load, ordinary = portions_of(amount, rows * top, bound, skew, True), portions_of(amount, rows * top, bound, skew, False)
    places = jnp.arange(amount)

    def named(lengths, offset_by):
        used = int((lengths > 0).sum())
        fixed = max(1, used // 4)
        passed = fixed + (places - fixed + offset_by * (used - fixed)) % max(1, amount - fixed)
        return jnp.zeros((amount,), jnp.int32).at[ranking[jnp.where(places < fixed, places, passed)]].set(jnp.asarray(lengths, jnp.int32))

    lengths = jnp.where(number % 4 == 0, named(heavy_load, number // 4), named(ordinary, number - number // 4 - 1))
    mixed = jax.random.permutation(jax.random.fold_in(own, 3), amount)
    donor, sink = mixed[0:amount // 2 * 2:2], mixed[1:amount // 2 * 2:2]
    margin = jnp.minimum(lengths[donor] - 1, bound - lengths[sink]) // 2
    margin = jnp.where((donor == ranking[0]) | (sink == ranking[0]) | (lengths[sink] == 0), 0, jnp.maximum(margin, 0))
    passed = jax.random.randint(jax.random.fold_in(own, 4), (amount // 2,), 0, 1 << 20) % (margin + 1)
    lengths = lengths.at[donor].add(-passed).at[sink].add(passed)
    labels = jnp.searchsorted(jnp.cumsum(lengths), jnp.arange(rows * top), side="right").astype(jnp.int32)
    grid = labels.reshape(top, rows).T
    grid = grid[jax.random.permutation(jax.random.fold_in(own, 1), rows)]
    offset_by = jax.random.randint(jax.random.fold_in(own, 2), (rows, 1), 0, top)
    return jnp.take_along_axis(grid, (jnp.arange(top)[None, :] + offset_by) % top, axis=1)


def portions_of(count, total, reach, skew, full):
    portions = [(1 << 20) // math.isqrt(grade ** skew) + 1 for grade in range(1, count + 1)]
    largest = reach if full else min(reach, max(-(-total // count), total * portions[0] // sum(portions)))
    least = 1 if total - largest >= count - 1 else 0
    holding, surplus = [largest] + [least] * (count - 1), total - largest - least * (count - 1)
    while surplus > 0:
        movable = [i for i in range(1, count) if holding[i] < largest] or [i for i in range(1, count) if holding[i] < reach]
        pool, left = sum([portions[i] for i in movable]), surplus
        for i in movable:
            more = min(reach - holding[i], max(1, left * portions[i] // pool), surplus)
            holding[i] = holding[i] + more
            surplus = surplus - more
    return np.array(holding)


def bell_draw(own_key, dims, deviation, bound, shards=(), kind=jnp.bfloat16):
    gain = block_scale(own_key, dims, shards, -0.22, 0.18) if shards else 1.0
    array = jax.random.normal(own_key, dims, jnp.float32) * deviation * gain
    return jnp.minimum(jnp.maximum(array, -bound), bound).astype(kind)


def setup_inputs(seed: int = 0) -> dict:
    key_of = jax.random.split(jax.random.key(seed), 9)
    tokens = bell_draw(key_of[0], (TOKENS, D), 1.0, 6.0, ((0, 4),))
    cotangent = bell_draw(key_of[1], (TOKENS, D), 1.0, 6.0, ((0, 4),))
    group_prob = jnp.clip(0.25 + 0.75 * jax.random.uniform(key_of[2], (TOKENS,), jnp.float32) ** block_scale(key_of[2], (TOKENS,), ((0, 4),), -0.2, 0.2), 0.25, 1.0)
    expert_prob = jnp.clip(0.1 + 0.9 * jax.random.uniform(key_of[3], (TOKENS, TOP_K), jnp.float32) ** block_scale(key_of[3], (TOKENS, TOP_K), ((0, 4),), -0.2, 0.2), 0.1, 1.0)
    routing_keys = jax.random.split(jax.random.fold_in(key_of[4], 1), TOKENS // TOK_DEV)
    routing_turns = jax.random.permutation(jax.random.fold_in(key_of[4], 3), TOKENS // TOK_DEV)
    routing = jax.vmap(lambda own, number: assign_block(jax.random.fold_in(key_of[4], 2), own, number, TOK_DEV, EXPERTS, TOP_K, CAP, 2))(routing_keys, routing_turns).reshape((TOKENS, TOP_K))
    gate_weight = bell_draw(key_of[5], (EXPERTS, D, FF), D ** -0.5, 0.125, ((0, 4), (2, 8)))
    up_weight = bell_draw(key_of[6], (EXPERTS, D, FF), D ** -0.5, 0.125, ((0, 4), (2, 8)))
    down_weight = draw_down_weight(jax.random.fold_in(key_of[8], 71), 0)
    return {"tokens": tokens, "cotangent": cotangent, "group_prob": group_prob, "expert_prob": expert_prob, "routing": routing, "gate_weight": gate_weight, "up_weight": up_weight, "down_weight": down_weight}


def slot_targets(route_block):
    flat = route_block.reshape(-1).astype(jnp.int32)
    names = jnp.arange(EXPERTS, dtype=jnp.int32)
    onehot = (flat[:, None] == names[None, :]).astype(jnp.int32)
    before = (jnp.cumsum(onehot, axis=0) - onehot).astype(jnp.int32)
    place = jnp.sum(before * onehot, axis=1).astype(jnp.int32)
    return (flat * CAP + place).astype(jnp.int32)


def expert_pass(operands):
    rows_in, rows_scaled, w_gate, w_up, w_down = operands
    pre_gate = jnp.dot(rows_in, w_gate, preferred_element_type=jnp.float32)
    pre_up = jnp.dot(rows_in, w_up, preferred_element_type=jnp.float32)
    sigma = jax.nn.sigmoid(pre_gate)
    activated = pre_gate * sigma
    derivative = sigma * (1.0 + pre_gate * (1.0 - sigma))
    hidden = (activated * pre_up).astype(jnp.bfloat16)
    hidden_grad = jnp.dot(rows_scaled, w_down.T, preferred_element_type=jnp.float32)
    score = jnp.sum(hidden.astype(jnp.float32) * hidden_grad, axis=1)
    gate_pre = (hidden_grad * pre_up * derivative).astype(jnp.bfloat16)
    up_pre = (hidden_grad * activated).astype(jnp.bfloat16)
    down_sum = jnp.dot(hidden.T, rows_scaled, preferred_element_type=jnp.float32)
    gate_sum = jnp.dot(rows_in.T, gate_pre, preferred_element_type=jnp.float32)
    up_sum = jnp.dot(rows_in.T, up_pre, preferred_element_type=jnp.float32)
    slot_grad = jnp.dot(gate_pre, w_gate.T, preferred_element_type=jnp.float32)
    slot_grad = (slot_grad + jnp.dot(up_pre, w_up.T, preferred_element_type=jnp.float32)).astype(jnp.bfloat16)
    gate_norm = jnp.sum(gate_sum * gate_sum, axis=1) / FF
    up_norm = jnp.sum(up_sum * up_sum, axis=1) / FF
    down_norm = jnp.sum(down_sum * down_sum, axis=1) / D
    return (slot_grad, score, gate_sum.astype(jnp.bfloat16), up_sum.astype(jnp.bfloat16),
            down_sum.astype(jnp.bfloat16), gate_norm, up_norm, down_norm)


def to_experts(buffer):
    tail = buffer.shape[2:]
    shaped = buffer.reshape((N_EP, EXPERTS, CAP) + tail)
    shaped = jnp.swapaxes(shaped, 0, 1)
    return shaped.reshape((EXPERTS, N_EP * CAP) + tail)


def to_blocks(buffer):
    tail = buffer.shape[2:]
    shaped = buffer.reshape((EXPERTS, N_EP, CAP) + tail)
    shaped = jnp.swapaxes(shaped, 0, 1)
    return shaped.reshape((N_EP, EXPERTS * CAP) + tail)


def reference(tokens, cotangent, group_prob, expert_prob, routing, gate_weight, up_weight, down_weight):
    slot_count = TOK_DEV * TOP_K
    blocks = routing.reshape(N_EP, TOK_DEV, TOP_K)
    target = jax.vmap(slot_targets)(blocks)
    source = jnp.broadcast_to(jnp.arange(N_EP, dtype=jnp.int32)[:, None], target.shape)
    weight = group_prob[:, None] * expert_prob
    scaled = (weight[:, :, None] * cotangent.astype(jnp.float32)[:, None, :]).astype(jnp.bfloat16)
    token_slots = jnp.broadcast_to(tokens.reshape(N_EP, TOK_DEV, 1, D), (N_EP, TOK_DEV, TOP_K, D))
    token_slots = token_slots.reshape(N_EP, slot_count, D)
    scaled_slots = scaled.reshape(N_EP, slot_count, D)
    rows_in = jnp.zeros((N_EP, EXPERTS * CAP, D), jnp.bfloat16).at[source, target].set(token_slots)
    rows_scaled = jnp.zeros((N_EP, EXPERTS * CAP, D), jnp.bfloat16).at[source, target].set(scaled_slots)
    results = lax.map(expert_pass, (to_experts(rows_in), to_experts(rows_scaled), gate_weight, up_weight, down_weight))
    slot_grad, score, gate_grad, up_grad, down_grad, gate_norm, up_norm, down_norm = results
    returned = to_blocks(slot_grad)
    per_slot = jnp.take_along_axis(returned, target[:, :, None], axis=1)
    per_slot = per_slot.astype(jnp.float32).reshape(N_EP * TOK_DEV, TOP_K, D)
    token_grad = jnp.sum(per_slot, axis=1).astype(jnp.bfloat16)
    score_back = jnp.take_along_axis(to_blocks(score), target, axis=1).reshape(N_EP * TOK_DEV, TOP_K)
    slot_score = score_back / weight
    expert_prob_grad = group_prob[:, None] * slot_score
    group_prob_grad = jnp.sum(expert_prob * slot_score, axis=1)
    return (token_grad, group_prob_grad, expert_prob_grad, gate_grad, up_grad, down_grad,
            gate_norm, up_norm, down_norm)
```

```python
import functools
import jax
import jax.numpy as jnp
from jax import lax
from jax.experimental import pallas as pl
from jax.experimental.pallas import tpu as pltpu
from jax.sharding import PartitionSpec as P

MESH = pl.DeviceIdType.MESH
CHUNKS = 4


def dispatch_kernel(n_ep, mine_ref, out_ref, local_sem, send_sem, recv_sem, fwd_send, fwd_recv):
    me = lax.axis_index("ep")
    t = lax.axis_index("tp")
    core = lax.rem(t, 2)
    partner = t + 1 - 2 * core
    width = mine_ref.shape[2] // CHUNKS
    barrier = pltpu.get_barrier_semaphore()
    for d in range(1, n_ep):
        pl.semaphore_signal(
            barrier, inc=1, device_id={"ep": lax.rem(me + d, n_ep)}, device_id_type=MESH
        )
    pl.semaphore_signal(barrier, inc=1, device_id={"tp": partner}, device_id_type=MESH)
    pl.semaphore_wait(barrier, n_ep)

    def cols(c):
        return pl.ds(c * width, width)

    def to_peer(d, c):
        dst = lax.rem(me + d, n_ep)
        return pltpu.make_async_remote_copy(
            src_ref=mine_ref.at[dst, :, cols(c)],
            dst_ref=out_ref.at[core, me, :, cols(c)],
            send_sem=send_sem.at[d, c],
            recv_sem=recv_sem.at[d, c],
            device_id={"ep": dst},
            device_id_type=MESH,
        )

    def from_peer(d, c):
        src = lax.rem(me - d + n_ep, n_ep)
        return pltpu.make_async_remote_copy(
            src_ref=mine_ref.at[me, :, cols(c)],
            dst_ref=out_ref.at[core, src, :, cols(c)],
            send_sem=send_sem.at[d, c],
            recv_sem=recv_sem.at[d, c],
            device_id={"ep": src},
            device_id_type=MESH,
        )

    def forward(d, c, side):
        src = lax.rem(me - d + n_ep, n_ep)
        source = mine_ref.at[me, :, cols(c)] if d == 0 else out_ref.at[side, src, :, cols(c)]
        return pltpu.make_async_remote_copy(
            src_ref=source,
            dst_ref=out_ref.at[side, src, :, cols(c)],
            send_sem=fwd_send.at[d, c],
            recv_sem=fwd_recv.at[d, c],
            device_id={"tp": partner},
            device_id_type=MESH,
        )

    order = sorted(range(1, n_ep), key=lambda d: abs(d - n_ep // 2))
    for c in range(CHUNKS):
        for d in order:
            to_peer(d, c).start()
    keep = pltpu.make_async_copy(mine_ref.at[me], out_ref.at[core, me], local_sem)
    keep.start()
    for c in range(CHUNKS):
        forward(0, c, core).start()
    for c in range(CHUNKS):
        for d in order:
            from_peer(d, c).wait_recv()
            forward(d, c, core).start()
    keep.wait()
    for c in range(CHUNKS):
        for d in order:
            to_peer(d, c).wait_send()
    for d in range(n_ep):
        for c in range(CHUNKS):
            forward(d, c, core).wait_send()
            forward(d, c, 1 - core).wait_recv()


def dispatch(mine, n_ep):
    return pl.pallas_call(
        functools.partial(dispatch_kernel, n_ep),
        out_shape=jax.ShapeDtypeStruct((2,) + mine.shape, mine.dtype),
        in_specs=[pl.BlockSpec(memory_space=pltpu.VMEM)],
        out_specs=pl.BlockSpec(memory_space=pl.ANY),
        scratch_shapes=[
            pltpu.SemaphoreType.DMA,
            pltpu.SemaphoreType.DMA((n_ep, CHUNKS)),
            pltpu.SemaphoreType.DMA((n_ep, CHUNKS)),
            pltpu.SemaphoreType.DMA((n_ep, CHUNKS)),
            pltpu.SemaphoreType.DMA((n_ep, CHUNKS)),
        ],
        compiler_params=pltpu.CompilerParams(collective_id=0, has_side_effects=True),
        name="dispatch",
    )(mine)


def sums_kernel(n_ep, n_tp, part_ref, norm_ref, score_ref, slots, total, send_sem, recv_sem, s_send, s_recv):
    me = lax.axis_index("ep")
    t = lax.axis_index("tp")
    barrier = pltpu.get_barrier_semaphore()
    for d in range(1, n_tp):
        pl.semaphore_signal(
            barrier, inc=1, device_id={"tp": lax.rem(t + d, n_tp)}, device_id_type=MESH
        )
    for d in range(1, n_ep):
        pl.semaphore_signal(
            barrier, inc=1, device_id={"ep": lax.rem(me + d, n_ep)}, device_id_type=MESH
        )
    pl.semaphore_wait(barrier, n_tp - 1 + n_ep - 1)

    def part_to(d):
        return pltpu.make_async_remote_copy(
            src_ref=part_ref,
            dst_ref=slots.at[t],
            send_sem=send_sem.at[d],
            recv_sem=recv_sem.at[d],
            device_id={"tp": lax.rem(t + d, n_tp)},
            device_id_type=MESH,
        )

    def part_from(d):
        src = lax.rem(t - d + n_tp, n_tp)
        return pltpu.make_async_remote_copy(
            src_ref=part_ref,
            dst_ref=slots.at[src],
            send_sem=send_sem.at[d],
            recv_sem=recv_sem.at[d],
            device_id={"tp": src},
            device_id_type=MESH,
        )

    for d in range(1, n_tp):
        part_to(d).start()
    slots[t] = part_ref[...]
    for d in range(1, n_tp):
        part_from(d).wait_recv()
    acc = slots[0]
    for i in range(1, n_tp):
        acc = acc + slots[i]
    total[...] = acc
    rows = 8 * n_ep

    def score_to(d):
        dst = lax.rem(me + d, n_ep)
        return pltpu.make_async_remote_copy(
            src_ref=total.at[pl.ds(pl.multiple_of(dst * 8, 8), 8)],
            dst_ref=score_ref.at[me],
            send_sem=s_send.at[d],
            recv_sem=s_recv.at[d],
            device_id={"ep": dst},
            device_id_type=MESH,
        )

    def score_from(d):
        src = lax.rem(me - d + n_ep, n_ep)
        return pltpu.make_async_remote_copy(
            src_ref=total.at[pl.ds(0, 8)],
            dst_ref=score_ref.at[src],
            send_sem=s_send.at[d],
            recv_sem=s_recv.at[d],
            device_id={"ep": src},
            device_id_type=MESH,
        )

    norm_ref[...] = acc[rows:]
    for d in range(1, n_tp):
        part_to(d).wait_send()
    for d in range(1, n_ep):
        score_to(d).start()
    score_ref[me] = total[pl.ds(pl.multiple_of(me * 8, 8), 8)]
    for d in range(1, n_ep):
        score_from(d).wait_recv()
    for d in range(1, n_ep):
        score_to(d).wait_send()


def small_sums(scores, norms, n_ep, n_tp):
    cap = scores.shape[1]
    width = norms.shape[1]
    padded = jnp.pad(scores, ((0, 0), (0, 1024 - cap))).reshape(n_ep * 8, 128)
    part = jnp.concatenate([padded, norms.reshape(2 * width // 128, 128)], axis=0)
    norm_out, score_out = pl.pallas_call(
        functools.partial(sums_kernel, n_ep, n_tp),
        out_shape=(
            jax.ShapeDtypeStruct((2 * width // 128, 128), jnp.float32),
            jax.ShapeDtypeStruct((n_ep, 8, 128), jnp.float32),
        ),
        in_specs=[pl.BlockSpec(memory_space=pltpu.VMEM)],
        out_specs=(
            pl.BlockSpec(memory_space=pltpu.VMEM),
            pl.BlockSpec(memory_space=pltpu.VMEM),
        ),
        scratch_shapes=[
            pltpu.VMEM((n_tp,) + part.shape, jnp.float32),
            pltpu.VMEM(part.shape, jnp.float32),
            pltpu.SemaphoreType.DMA((n_tp,)),
            pltpu.SemaphoreType.DMA((n_tp,)),
            pltpu.SemaphoreType.DMA((n_ep,)),
            pltpu.SemaphoreType.DMA((n_ep,)),
        ],
        compiler_params=pltpu.CompilerParams(collective_id=1, has_side_effects=True),
        cost_estimate=pl.CostEstimate(flops=0, bytes_accessed=20_000_000, transcendentals=0),
        name="small_sums",
    )(part)
    return score_out.reshape(n_ep, 1024)[:, :cap], norm_out.reshape(2, width)


def local(tokens, cotangent, group_prob, expert_prob, routing, gate_weight, up_weight, down_weight):
    tok_count, model_width = tokens.shape
    top_count = routing.shape[1]
    n_ep = lax.axis_size("ep")
    n_tp = lax.axis_size("tp")
    capacity = 3 * tok_count * top_count // (2 * n_ep)
    buffer_rows = n_ep * capacity
    core = lax.rem(lax.axis_index("tp"), 2)
    weight = group_prob[:, None] * expert_prob

    experts = jnp.arange(n_ep, dtype=jnp.int32)[:, None]
    picks = [routing[None, :, k] == experts for k in range(top_count)]
    named = functools.reduce(jnp.logical_or, picks)
    weight_of = sum(jnp.where(picks[k], weight[None, :, k], 0.0) for k in range(top_count))
    earlier = (
        lax.broadcasted_iota(jnp.int32, (tok_count, tok_count), 0)
        < lax.broadcasted_iota(jnp.int32, (tok_count, tok_count), 1)
    ).astype(jnp.bfloat16)
    before = jnp.dot(named.astype(jnp.bfloat16), earlier, preferred_element_type=jnp.float32)
    place = jnp.where(named, before.astype(jnp.int32), -1)
    filled = place[:, None, :] == lax.broadcasted_iota(jnp.int32, (n_ep, capacity, tok_count), 1)
    pick = filled.astype(jnp.bfloat16).reshape(buffer_rows, tok_count)
    slot_weight = jnp.sum(jnp.where(filled, weight_of[:, None, :], 0.0), axis=2).reshape(buffer_rows, 1)

    source = jnp.where(core == 0, tokens, cotangent)
    factor = jnp.where(core == 0, 1.0, slot_weight)
    mine = jnp.dot(pick, source, preferred_element_type=jnp.float32) * factor
    mine = mine.astype(jnp.bfloat16).reshape(n_ep, capacity, model_width)
    both = dispatch(mine, n_ep)
    flat_in = both[0].reshape(buffer_rows, model_width)
    flat_scaled = both[1].reshape(buffer_rows, model_width)

    w_gate = gate_weight[0]
    w_up = up_weight[0]
    w_down = down_weight[0]
    hidden_total = gate_weight.shape[2] * n_tp
    contract_last = (((1,), (1,)), ((), ()))
    contract_rows = (((0,), (0,)), ((), ()))
    pre_gate = jnp.dot(flat_in, w_gate, preferred_element_type=jnp.float32)
    pre_up = jnp.dot(flat_in, w_up, preferred_element_type=jnp.float32)
    sigma = jax.nn.sigmoid(pre_gate)
    activated = pre_gate * sigma
    derivative = sigma * (1.0 + pre_gate * (1.0 - sigma))
    hidden = (activated * pre_up).astype(jnp.bfloat16)
    hidden_grad = lax.dot_general(
        flat_scaled, w_down, contract_last, preferred_element_type=jnp.float32
    )
    score_part = jnp.sum(hidden.astype(jnp.float32) * hidden_grad, axis=1).reshape(n_ep, capacity)
    gate_pre = (hidden_grad * pre_up * derivative).astype(jnp.bfloat16)
    up_pre = (hidden_grad * activated).astype(jnp.bfloat16)
    input_part = lax.dot_general(
        gate_pre, w_gate, contract_last, preferred_element_type=jnp.float32
    )
    input_part = input_part + lax.dot_general(
        up_pre, w_up, contract_last, preferred_element_type=jnp.float32
    )
    input_part = input_part.astype(jnp.bfloat16).reshape(n_ep, capacity, model_width)
    share = lax.psum_scatter(input_part, "tp", scatter_dimension=2, tiled=True)

    down_sum = lax.dot_general(
        hidden, flat_scaled, contract_rows, preferred_element_type=jnp.float32
    )
    gate_sum = lax.dot_general(flat_in, gate_pre, contract_rows, preferred_element_type=jnp.float32)
    up_sum = lax.dot_general(flat_in, up_pre, contract_rows, preferred_element_type=jnp.float32)
    norm_part = (
        jnp.stack([jnp.sum(gate_sum * gate_sum, axis=1), jnp.sum(up_sum * up_sum, axis=1)])
        / hidden_total
    )
    down_norms = jnp.sum(down_sum * down_sum, axis=1) / model_width
    scores, row_norms = small_sums(score_part, norm_part, n_ep, n_tp)

    share, scores, row_norms, down_norms = lax.optimization_barrier(
        (share, scores, row_norms, down_norms)
    )
    returned = lax.all_to_all(share, "ep", split_axis=0, concat_axis=0, tiled=True)
    returned = returned.reshape(buffer_rows, -1)
    token_share = lax.dot_general(pick, returned, contract_rows, preferred_element_type=jnp.float32)
    token_grad = lax.all_gather(token_share.astype(jnp.bfloat16), "tp", axis=1, tiled=True)

    score_of = jnp.sum(jnp.where(filled, scores[:, :, None], 0.0), axis=1)
    slot_score = jnp.stack(
        [jnp.sum(jnp.where(p, score_of, 0.0), axis=0) for p in picks], axis=1
    ) / weight
    expert_prob_grad = group_prob[:, None] * slot_score
    group_prob_grad = jnp.sum(expert_prob * slot_score, axis=1)
    return (
        token_grad,
        group_prob_grad,
        expert_prob_grad,
        gate_sum.astype(jnp.bfloat16)[None],
        up_sum.astype(jnp.bfloat16)[None],
        down_sum.astype(jnp.bfloat16)[None],
        row_norms[0][None],
        row_norms[1][None],
        down_norms[None],
    )


def solution(mesh):
    return jax.shard_map(
        local,
        mesh=mesh,
        in_specs=(
            P("ep", None),
            P("ep", None),
            P("ep"),
            P("ep", None),
            P("ep", None),
            P("ep", None, "tp"),
            P("ep", None, "tp"),
            P("ep", "tp", None),
        ),
        out_specs=(
            P("ep", None),
            P("ep"),
            P("ep", None),
            P("ep", None, "tp"),
            P("ep", None, "tp"),
            P("ep", "tp", None),
            P("ep", None),
            P("ep", None),
            P("ep", "tp"),
        ),
        check_vma=False,
    )
```

```python
import functools
import jax
import jax.numpy as jnp
from jax import lax
from jax.experimental import pallas as pl
from jax.experimental.pallas import tpu as pltpu
from jax.sharding import PartitionSpec as P

MESH = pl.DeviceIdType.MESH
CHUNKS = 4


def dispatch_kernel(n_ep, mine_ref, out_ref, local_sem, send_sem, recv_sem, fwd_send, fwd_recv):
    me = lax.axis_index("ep")
    t = lax.axis_index("tp")
    core = lax.rem(t, 2)
    partner = t + 1 - 2 * core
    width = mine_ref.shape[2] // CHUNKS
    barrier = pltpu.get_barrier_semaphore()
    for d in range(1, n_ep):
        pl.semaphore_signal(
            barrier, inc=1, device_id={"ep": lax.rem(me + d, n_ep)}, device_id_type=MESH
        )
    pl.semaphore_signal(barrier, inc=1, device_id={"tp": partner}, device_id_type=MESH)
    pl.semaphore_wait(barrier, n_ep)

    def cols(c):
        return pl.ds(c * width, width)

    def to_peer(d, c):
        dst = lax.rem(me + d, n_ep)
        return pltpu.make_async_remote_copy(
            src_ref=mine_ref.at[dst, :, cols(c)],
            dst_ref=out_ref.at[core, me, :, cols(c)],
            send_sem=send_sem.at[d, c],
            recv_sem=recv_sem.at[d, c],
            device_id={"ep": dst},
            device_id_type=MESH,
        )

    def from_peer(d, c):
        src = lax.rem(me - d + n_ep, n_ep)
        return pltpu.make_async_remote_copy(
            src_ref=mine_ref.at[me, :, cols(c)],
            dst_ref=out_ref.at[core, src, :, cols(c)],
            send_sem=send_sem.at[d, c],
            recv_sem=recv_sem.at[d, c],
            device_id={"ep": src},
            device_id_type=MESH,
        )

    def forward(d, c, side):
        src = lax.rem(me - d + n_ep, n_ep)
        source = mine_ref.at[me, :, cols(c)] if d == 0 else out_ref.at[side, src, :, cols(c)]
        return pltpu.make_async_remote_copy(
            src_ref=source,
            dst_ref=out_ref.at[side, src, :, cols(c)],
            send_sem=fwd_send.at[d, c],
            recv_sem=fwd_recv.at[d, c],
            device_id={"tp": partner},
            device_id_type=MESH,
        )

    order = sorted(range(1, n_ep), key=lambda d: abs(d - n_ep // 2))
    for c in range(CHUNKS):
        for d in order:
            to_peer(d, c).start()
    keep = pltpu.make_async_copy(mine_ref.at[me], out_ref.at[core, me], local_sem)
    keep.start()
    for c in range(CHUNKS):
        forward(0, c, core).start()
    for c in range(CHUNKS):
        for d in order:
            from_peer(d, c).wait_recv()
            forward(d, c, core).start()
    keep.wait()
    for c in range(CHUNKS):
        for d in order:
            to_peer(d, c).wait_send()
    for d in range(n_ep):
        for c in range(CHUNKS):
            forward(d, c, core).wait_send()
            forward(d, c, 1 - core).wait_recv()


def dispatch(mine, n_ep):
    return pl.pallas_call(
        functools.partial(dispatch_kernel, n_ep),
        out_shape=jax.ShapeDtypeStruct((2,) + mine.shape, mine.dtype),
        in_specs=[pl.BlockSpec(memory_space=pltpu.VMEM)],
        out_specs=pl.BlockSpec(memory_space=pl.ANY),
        scratch_shapes=[
            pltpu.SemaphoreType.DMA,
            pltpu.SemaphoreType.DMA((n_ep, CHUNKS)),
            pltpu.SemaphoreType.DMA((n_ep, CHUNKS)),
            pltpu.SemaphoreType.DMA((n_ep, CHUNKS)),
            pltpu.SemaphoreType.DMA((n_ep, CHUNKS)),
        ],
        compiler_params=pltpu.CompilerParams(collective_id=0, has_side_effects=True),
        name="dispatch",
    )(mine)


def sums_kernel(n_ep, n_tp, part_ref, norm_ref, score_ref, slots, total, send_sem, recv_sem, s_send, s_recv):
    me = lax.axis_index("ep")
    t = lax.axis_index("tp")
    barrier = pltpu.get_barrier_semaphore()
    for d in range(1, n_tp):
        pl.semaphore_signal(
            barrier, inc=1, device_id={"tp": lax.rem(t + d, n_tp)}, device_id_type=MESH
        )
    for d in range(1, n_ep):
        pl.semaphore_signal(
            barrier, inc=1, device_id={"ep": lax.rem(me + d, n_ep)}, device_id_type=MESH
        )
    pl.semaphore_wait(barrier, n_tp - 1 + n_ep - 1)

    def part_to(d):
        return pltpu.make_async_remote_copy(
            src_ref=part_ref,
            dst_ref=slots.at[t],
            send_sem=send_sem.at[d],
            recv_sem=recv_sem.at[d],
            device_id={"tp": lax.rem(t + d, n_tp)},
            device_id_type=MESH,
        )

    def part_from(d):
        src = lax.rem(t - d + n_tp, n_tp)
        return pltpu.make_async_remote_copy(
            src_ref=part_ref,
            dst_ref=slots.at[src],
            send_sem=send_sem.at[d],
            recv_sem=recv_sem.at[d],
            device_id={"tp": src},
            device_id_type=MESH,
        )

    for d in range(1, n_tp):
        part_to(d).start()
    slots[t] = part_ref[...]
    for d in range(1, n_tp):
        part_from(d).wait_recv()
    acc = slots[0]
    for i in range(1, n_tp):
        acc = acc + slots[i]
    total[...] = acc
    rows = 8 * n_ep

    def score_to(d):
        dst = lax.rem(me + d, n_ep)
        return pltpu.make_async_remote_copy(
            src_ref=total.at[pl.ds(pl.multiple_of(dst * 8, 8), 8)],
            dst_ref=score_ref.at[me],
            send_sem=s_send.at[d],
            recv_sem=s_recv.at[d],
            device_id={"ep": dst},
            device_id_type=MESH,
        )

    def score_from(d):
        src = lax.rem(me - d + n_ep, n_ep)
        return pltpu.make_async_remote_copy(
            src_ref=total.at[pl.ds(0, 8)],
            dst_ref=score_ref.at[src],
            send_sem=s_send.at[d],
            recv_sem=s_recv.at[d],
            device_id={"ep": src},
            device_id_type=MESH,
        )

    norm_ref[...] = acc[rows:]
    for d in range(1, n_tp):
        part_to(d).wait_send()
    for d in range(1, n_ep):
        score_to(d).start()
    score_ref[me] = total[pl.ds(pl.multiple_of(me * 8, 8), 8)]
    for d in range(1, n_ep):
        score_from(d).wait_recv()
    for d in range(1, n_ep):
        score_to(d).wait_send()


def small_sums(scores, norms, n_ep, n_tp):
    cap = scores.shape[1]
    width = norms.shape[1]
    padded = jnp.pad(scores, ((0, 0), (0, 1024 - cap))).reshape(n_ep * 8, 128)
    part = jnp.concatenate([padded, norms.reshape(2 * width // 128, 128)], axis=0)
    norm_out, score_out = pl.pallas_call(
        functools.partial(sums_kernel, n_ep, n_tp),
        out_shape=(
            jax.ShapeDtypeStruct((2 * width // 128, 128), jnp.float32),
            jax.ShapeDtypeStruct((n_ep, 8, 128), jnp.float32),
        ),
        in_specs=[pl.BlockSpec(memory_space=pltpu.VMEM)],
        out_specs=(
            pl.BlockSpec(memory_space=pltpu.VMEM),
            pl.BlockSpec(memory_space=pltpu.VMEM),
        ),
        scratch_shapes=[
            pltpu.VMEM((n_tp,) + part.shape, jnp.float32),
            pltpu.VMEM(part.shape, jnp.float32),
            pltpu.SemaphoreType.DMA((n_tp,)),
            pltpu.SemaphoreType.DMA((n_tp,)),
            pltpu.SemaphoreType.DMA((n_ep,)),
            pltpu.SemaphoreType.DMA((n_ep,)),
        ],
        compiler_params=pltpu.CompilerParams(collective_id=1, has_side_effects=True),
        cost_estimate=pl.CostEstimate(flops=0, bytes_accessed=20_000_000, transcendentals=0),
        name="small_sums",
    )(part)
    return score_out.reshape(n_ep, 1024)[:, :cap], norm_out.reshape(2, width)


def finish_kernel(
    n_ep, n_tp, both_ref, gate_ref, up_ref, hid_ref, part_ref, score_ref, pick_ref,
    out_ref, gate_out, up_out, down_out, norm_ref, down_norm_ref, score_out,
    rows_in, rows_scaled, gate_v, up_v, hid_v, gate_g, up_g, down_g, norm_part,
    s_slots, s_total, n_slots, bufs, accs, returned,
    load_sem, store_sem, rs_send, rs_recv, ep_send, ep_recv, ag_send, ag_recv,
    sc_send, sc_recv, sx_send, sx_recv, nm_send, nm_recv,
):
    me = lax.axis_index("ep")
    t = lax.axis_index("tp")
    cap, width = part_ref.shape[1], part_ref.shape[2]
    ff = gate_v.shape[1]
    tok = out_ref.shape[0]
    levels = len(bufs)
    bits = [lax.rem(t // (1 << s), 2) for s in range(levels)]
    peers = [t + (1 - 2 * bits[s]) * (1 << s) for s in range(levels)]

    def remote(src, dst, send, recv, device):
        return pltpu.make_async_remote_copy(
            src_ref=src, dst_ref=dst, send_sem=send, recv_sem=recv,
            device_id=device, device_id_type=MESH,
        )

    loads = []
    for b in range(n_ep):
        loads.append(pltpu.make_async_copy(
            both_ref.at[0, b], rows_in.at[pl.ds(b * cap, cap)], load_sem.at[len(loads)]))
        loads.append(pltpu.make_async_copy(
            both_ref.at[1, b], rows_scaled.at[pl.ds(b * cap, cap)], load_sem.at[len(loads)]))
    for src, dst in ((gate_ref, gate_v), (up_ref, up_v), (hid_ref, hid_v)):
        loads.append(pltpu.make_async_copy(src, dst, load_sem.at[len(loads)]))

    barrier = pltpu.get_barrier_semaphore()
    for d in range(1, n_tp):
        pl.semaphore_signal(
            barrier, inc=1, device_id={"tp": lax.rem(t + d, n_tp)}, device_id_type=MESH
        )
    for d in range(1, n_ep):
        pl.semaphore_signal(
            barrier, inc=1, device_id={"ep": lax.rem(me + d, n_ep)}, device_id_type=MESH
        )
    pl.semaphore_wait(barrier, n_tp - 1 + n_ep - 1)

    order = sorted(range(1, n_ep), key=lambda d: abs(d - n_ep // 2)) + [0]

    def block(i):
        return lax.rem(me + order[i], n_ep)

    def halves(s):
        w = width >> (s + 1)
        keep = pl.ds(pl.multiple_of(bits[s] * w, 128), w)
        give = pl.ds(pl.multiple_of((1 - bits[s]) * w, 128), w)
        return keep, give

    def exchange(s, i):
        _, give = halves(s)
        src = part_ref.at[block(i), :, give] if s == 0 else accs[s - 1].at[i, :, give]
        return remote(src, bufs[s].at[i], rs_send.at[s, i], rs_recv.at[s, i], {"tp": peers[s]})

    def to_owner(i):
        d = order[i]
        return remote(
            accs[levels - 1].at[i],
            returned.at[pl.ds(pl.multiple_of(me * cap, 16), cap)],
            ep_send.at[d], ep_recv.at[d], {"ep": block(i)},
        )

    def from_owner(d):
        src = lax.rem(me - d + n_ep, n_ep)
        return remote(
            accs[levels - 1].at[0],
            returned.at[pl.ds(pl.multiple_of(src * cap, 16), cap)],
            ep_send.at[d], ep_recv.at[d], {"ep": src},
        )

    def score_to(d):
        return remote(score_ref, s_slots.at[t], sc_send.at[d], sc_recv.at[d],
                      {"tp": lax.rem(t + d, n_tp)})

    def score_from(d):
        src = lax.rem(t - d + n_tp, n_tp)
        return remote(score_ref, s_slots.at[src], sc_send.at[d], sc_recv.at[d], {"tp": src})

    def norm_to(d):
        return remote(norm_part, n_slots.at[t], nm_send.at[d], nm_recv.at[d],
                      {"tp": lax.rem(t + d, n_tp)})

    def norm_from(d):
        src = lax.rem(t - d + n_tp, n_tp)
        return remote(norm_part, n_slots.at[src], nm_send.at[d], nm_recv.at[d], {"tp": src})

    def score_back(d):
        dst = lax.rem(me + d, n_ep)
        return remote(s_total.at[pl.ds(pl.multiple_of(dst * 8, 8), 8)], score_out.at[me],
                      sx_send.at[d], sx_recv.at[d], {"ep": dst})

    def score_arrive(d):
        src = lax.rem(me - d + n_ep, n_ep)
        return remote(s_total.at[pl.ds(0, 8)], score_out.at[src],
                      sx_send.at[d], sx_recv.at[d], {"ep": src})

    for i in range(n_ep):
        exchange(0, i).start()
    for d in range(1, n_tp):
        score_to(d).start()
    for copy in loads:
        copy.start()
    s_slots[t] = score_ref[...]

    rows = (((0,), (0,)), ((), ()))
    step = 256
    half = width // step // 2

    def fold(sq):
        parts = [sq[:, j * 128:(j + 1) * 128] for j in range(sq.shape[1] // 128)]
        return functools.reduce(jnp.add, parts)

    def line(x):
        return jnp.sum(jnp.transpose(x), axis=0, keepdims=True)

    def gate_up(first):
        def body(j, carry):
            at = pl.ds(pl.multiple_of(j * step, step), step)
            lhs = rows_in[:, at]
            for n, (rhs, out) in enumerate(((gate_v, gate_g), (up_v, up_g))):
                total = lax.dot_general(lhs, rhs[...], rows, preferred_element_type=jnp.float32)
                out[at, :] = total.astype(jnp.bfloat16)
                sq = fold(total * total)
                for h in range(step // 128):
                    norm_part[n, pl.ds(j * (step // 128) + h, 1), :] = line(
                        sq[h * 128:(h + 1) * 128]
                    ) / (ff * n_tp)
            return carry
        lax.fori_loop(first, first + half, body, 0)

    def down():
        def body(j, carry):
            at = pl.ds(pl.multiple_of(j * step, step), step)
            lhs = hid_v[:, at]
            sq = None
            for c in range(0, width, 512):
                total = lax.dot_general(
                    lhs, rows_scaled[:, c:c + 512], rows, preferred_element_type=jnp.float32
                )
                down_g[at, c:c + 512] = total.astype(jnp.bfloat16)
                more = fold(total * total)
                sq = more if sq is None else sq + more
            for h in range(step // 128):
                down_norm_ref[pl.ds(j * (step // 128) + h, 1), :] = line(
                    sq[h * 128:(h + 1) * 128]
                ) / width
            return carry
        lax.fori_loop(0, ff // step, body, 0)

    stores = [
        pltpu.make_async_copy(a, b, store_sem.at[n])
        for n, (a, b) in enumerate(((gate_g, gate_out), (up_g, up_out), (down_g, down_out)))
    ]

    def work_first():
        for copy in loads:
            copy.wait()
        gate_up(0)

    def work_second():
        gate_up(half)
        for d in range(1, n_tp):
            norm_to(d).start()
        n_slots[t] = norm_part[...]
        stores[0].start()
        stores[1].start()

    def work_third():
        for d in range(1, n_tp):
            score_from(d).wait_recv()
        acc = s_slots[0]
        for i in range(1, n_tp):
            acc = acc + s_slots[i]
        s_total[...] = acc
        down()
        stores[2].start()
        for d in range(1, n_ep):
            score_back(d).start()
        score_out[me] = s_total[pl.ds(pl.multiple_of(me * 8, 8), 8)]

    work = [work_first, work_second, work_third]
    for tick in range(max(n_ep + levels - 1, len(work))):
        for i in range(n_ep):
            s = tick - i
            if not 0 <= s < levels:
                continue
            exchange(s, i).wait_recv()
            keep, _ = halves(s)
            own = part_ref[block(i), :, keep] if s == 0 else accs[s - 1][i, :, keep]
            total = own.astype(jnp.float32) + bufs[s][i].astype(jnp.float32)
            accs[s][i] = total.astype(jnp.bfloat16)
            if s + 1 < levels:
                exchange(s + 1, i).start()
            elif order[i]:
                to_owner(i).start()
            else:
                returned[pl.ds(pl.multiple_of(me * cap, 16), cap), :] = total.astype(jnp.bfloat16)
        if tick < len(work):
            work[tick]()

    for d in range(1, n_ep):
        from_owner(d).wait_recv()
    share = width >> levels
    base = [None] * (levels + 1)
    base[0] = 0
    for s in range(levels):
        base[s + 1] = base[s] + bits[s] * (width >> (s + 1))
    pieces = 2
    piece = tok // pieces

    def spread(s, p):
        w = width >> (s + 1)
        at = pl.ds(pl.multiple_of(base[s + 1], 128), w)
        ref = out_ref.at[pl.ds(p * piece, piece), at]
        return remote(ref, ref, ag_send.at[s, p], ag_recv.at[s, p], {"tp": peers[s]})

    def arrived(s, p):
        w = width >> (s + 1)
        at = pl.ds(pl.multiple_of(base[s] + (1 - bits[s]) * w, 128), w)
        ref = out_ref.at[pl.ds(p * piece, piece), at]
        return remote(ref, ref, ag_send.at[s, p], ag_recv.at[s, p], {"tp": peers[s]})

    for p in range(pieces):
        grad = jnp.dot(
            pick_ref[p * piece:(p + 1) * piece, :], returned[...],
            preferred_element_type=jnp.float32,
        )
        out_ref[p * piece:(p + 1) * piece, pl.ds(pl.multiple_of(base[levels], 128), share)] = (
            grad.astype(jnp.bfloat16)
        )
        spread(levels - 1, p).start()
    for d in range(1, n_tp):
        norm_from(d).wait_recv()
    acc = n_slots[0]
    for i in range(1, n_tp):
        acc = acc + n_slots[i]
    norm_ref[...] = acc
    for s in reversed(range(levels)):
        for p in range(pieces):
            arrived(s, p).wait_recv()
            if s:
                spread(s - 1, p).start()

    for d in range(1, n_ep):
        score_arrive(d).wait_recv()
        score_back(d).wait_send()
    for i in range(n_ep):
        for s in range(levels):
            exchange(s, i).wait_send()
        if order[i]:
            to_owner(i).wait_send()
    for d in range(1, n_tp):
        score_to(d).wait_send()
        norm_to(d).wait_send()
    for s in range(levels):
        for p in range(pieces):
            spread(s, p).wait_send()
    for copy in stores:
        copy.wait()


def finish(both, gate_pre, up_pre, hidden, part, score_part, pick_t, n_ep, n_tp):
    cap, width = part.shape[1:]
    rows, ff = gate_pre.shape
    tok = pick_t.shape[0]
    levels = n_tp.bit_length() - 1
    scores = jnp.pad(score_part, ((0, 0), (0, 1024 - cap))).reshape(n_ep * 8, 128)
    bf, f32 = jnp.bfloat16, jnp.float32
    vmem = pl.BlockSpec(memory_space=pltpu.VMEM)
    hbm = pl.BlockSpec(memory_space=pl.ANY)
    dma = pltpu.SemaphoreType.DMA
    stages = [pltpu.VMEM((n_ep, cap, width >> (s + 1)), bf) for s in range(levels)]
    outs = pl.pallas_call(
        functools.partial(finish_kernel, n_ep, n_tp),
        out_shape=(
            jax.ShapeDtypeStruct((tok, width), bf),
            jax.ShapeDtypeStruct((width, ff), bf),
            jax.ShapeDtypeStruct((width, ff), bf),
            jax.ShapeDtypeStruct((ff, width), bf),
            jax.ShapeDtypeStruct((2, width // 128, 128), f32),
            jax.ShapeDtypeStruct((ff // 128, 128), f32),
            jax.ShapeDtypeStruct((n_ep, 8, 128), f32),
        ),
        in_specs=[hbm, hbm, hbm, hbm, vmem, vmem, vmem],
        out_specs=(vmem, hbm, hbm, hbm, vmem, vmem, vmem),
        scratch_shapes=[
            pltpu.VMEM((rows, width), bf),
            pltpu.VMEM((rows, width), bf),
            pltpu.VMEM((rows, ff), bf),
            pltpu.VMEM((rows, ff), bf),
            pltpu.VMEM((rows, ff), bf),
            pltpu.VMEM((width, ff), bf),
            pltpu.VMEM((width, ff), bf),
            pltpu.VMEM((ff, width), bf),
            pltpu.VMEM((2, width // 128, 128), f32),
            pltpu.VMEM((n_tp,) + scores.shape, f32),
            pltpu.VMEM(scores.shape, f32),
            pltpu.VMEM((n_tp, 2, width // 128, 128), f32),
            list(stages),
            list(stages),
            pltpu.VMEM((rows, width >> levels), bf),
            dma((2 * n_ep + 3,)),
            dma((3,)),
            dma((levels, n_ep)),
            dma((levels, n_ep)),
            dma((n_ep,)),
            dma((n_ep,)),
            dma((levels, 2)),
            dma((levels, 2)),
            dma((n_tp,)),
            dma((n_tp,)),
            dma((n_ep,)),
            dma((n_ep,)),
            dma((n_tp,)),
            dma((n_tp,)),
        ],
        compiler_params=pltpu.CompilerParams(
            collective_id=2, has_side_effects=True, vmem_limit_bytes=48 << 20
        ),
        name="finish",
    )(both, gate_pre, up_pre, hidden, part, scores, pick_t)
    token_grad, gate_g, up_g, down_g, norms, down_norms, score_out = outs
    return (
        token_grad, gate_g, up_g, down_g, norms.reshape(2, width),
        down_norms.reshape(ff), score_out.reshape(n_ep, 1024)[:, :cap],
    )


def local(tokens, cotangent, group_prob, expert_prob, routing, gate_weight, up_weight, down_weight):
    tok_count, model_width = tokens.shape
    top_count = routing.shape[1]
    n_ep = lax.axis_size("ep")
    n_tp = lax.axis_size("tp")
    capacity = 3 * tok_count * top_count // (2 * n_ep)
    buffer_rows = n_ep * capacity
    core = lax.rem(lax.axis_index("tp"), 2)
    weight = group_prob[:, None] * expert_prob

    experts = jnp.arange(n_ep, dtype=jnp.int32)[:, None]
    picks = [routing[None, :, k] == experts for k in range(top_count)]
    named = functools.reduce(jnp.logical_or, picks)
    weight_of = sum(jnp.where(picks[k], weight[None, :, k], 0.0) for k in range(top_count))
    earlier = (
        lax.broadcasted_iota(jnp.int32, (tok_count, tok_count), 0)
        < lax.broadcasted_iota(jnp.int32, (tok_count, tok_count), 1)
    ).astype(jnp.bfloat16)
    before = jnp.dot(named.astype(jnp.bfloat16), earlier, preferred_element_type=jnp.float32)
    place = jnp.where(named, before.astype(jnp.int32), -1)
    filled = place[:, None, :] == lax.broadcasted_iota(jnp.int32, (n_ep, capacity, tok_count), 1)
    pick = filled.astype(jnp.bfloat16).reshape(buffer_rows, tok_count)
    slot_weight = jnp.sum(jnp.where(filled, weight_of[:, None, :], 0.0), axis=2).reshape(buffer_rows, 1)

    source = jnp.where(core == 0, tokens, cotangent)
    factor = jnp.where(core == 0, 1.0, slot_weight)
    mine = jnp.dot(pick, source, preferred_element_type=jnp.float32) * factor
    mine = mine.astype(jnp.bfloat16).reshape(n_ep, capacity, model_width)
    both = dispatch(mine, n_ep)
    flat_in = both[0].reshape(buffer_rows, model_width)
    flat_scaled = both[1].reshape(buffer_rows, model_width)

    w_gate = gate_weight[0]
    w_up = up_weight[0]
    w_down = down_weight[0]
    hidden_total = gate_weight.shape[2] * n_tp
    contract_last = (((1,), (1,)), ((), ()))
    contract_rows = (((0,), (0,)), ((), ()))
    pre_gate = jnp.dot(flat_in, w_gate, preferred_element_type=jnp.float32)
    pre_up = jnp.dot(flat_in, w_up, preferred_element_type=jnp.float32)
    sigma = jax.nn.sigmoid(pre_gate)
    activated = pre_gate * sigma
    derivative = sigma * (1.0 + pre_gate * (1.0 - sigma))
    hidden = (activated * pre_up).astype(jnp.bfloat16)
    hidden_grad = lax.dot_general(
        flat_scaled, w_down, contract_last, preferred_element_type=jnp.float32
    )
    score_part = jnp.sum(hidden.astype(jnp.float32) * hidden_grad, axis=1).reshape(n_ep, capacity)
    gate_pre = (hidden_grad * pre_up * derivative).astype(jnp.bfloat16)
    up_pre = (hidden_grad * activated).astype(jnp.bfloat16)
    input_part = lax.dot_general(
        gate_pre, w_gate, contract_last, preferred_element_type=jnp.float32
    )
    input_part = input_part + lax.dot_general(
        up_pre, w_up, contract_last, preferred_element_type=jnp.float32
    )
    input_part = input_part.astype(jnp.bfloat16).reshape(n_ep, capacity, model_width)
    if n_tp & (n_tp - 1) == 0 and model_width // n_tp % 128 == 0:
        pick_t = pick.T
        token_grad, gate_grad, up_grad, down_grad, row_norms, down_norms, scores = finish(
            both, gate_pre, up_pre, hidden, input_part, score_part, pick_t, n_ep, n_tp
        )
    else:
        share = lax.psum_scatter(input_part, "tp", scatter_dimension=2, tiled=True)

        down_sum = lax.dot_general(
            hidden, flat_scaled, contract_rows, preferred_element_type=jnp.float32
        )
        gate_sum = lax.dot_general(flat_in, gate_pre, contract_rows, preferred_element_type=jnp.float32)
        up_sum = lax.dot_general(flat_in, up_pre, contract_rows, preferred_element_type=jnp.float32)
        norm_part = (
            jnp.stack([jnp.sum(gate_sum * gate_sum, axis=1), jnp.sum(up_sum * up_sum, axis=1)])
            / hidden_total
        )
        down_norms = jnp.sum(down_sum * down_sum, axis=1) / model_width
        scores, row_norms = small_sums(score_part, norm_part, n_ep, n_tp)

        share, scores, row_norms, down_norms = lax.optimization_barrier(
            (share, scores, row_norms, down_norms)
        )
        returned = lax.all_to_all(share, "ep", split_axis=0, concat_axis=0, tiled=True)
        returned = returned.reshape(buffer_rows, -1)
        token_share = lax.dot_general(pick, returned, contract_rows, preferred_element_type=jnp.float32)
        token_grad = lax.all_gather(token_share.astype(jnp.bfloat16), "tp", axis=1, tiled=True)
        gate_grad, up_grad, down_grad = (
            x.astype(jnp.bfloat16) for x in (gate_sum, up_sum, down_sum)
        )

    score_of = jnp.sum(jnp.where(filled, scores[:, :, None], 0.0), axis=1)
    slot_score = jnp.stack(
        [jnp.sum(jnp.where(p, score_of, 0.0), axis=0) for p in picks], axis=1
    ) / weight
    expert_prob_grad = group_prob[:, None] * slot_score
    group_prob_grad = jnp.sum(expert_prob * slot_score, axis=1)
    return (
        token_grad,
        group_prob_grad,
        expert_prob_grad,
        gate_grad[None],
        up_grad[None],
        down_grad[None],
        row_norms[0][None],
        row_norms[1][None],
        down_norms[None],
    )


def solution(mesh):
    return jax.shard_map(
        local,
        mesh=mesh,
        in_specs=(
            P("ep", None),
            P("ep", None),
            P("ep"),
            P("ep", None),
            P("ep", None),
            P("ep", None, "tp"),
            P("ep", None, "tp"),
            P("ep", "tp", None),
        ),
        out_specs=(
            P("ep", None),
            P("ep"),
            P("ep", None),
            P("ep", None, "tp"),
            P("ep", None, "tp"),
            P("ep", "tp", None),
            P("ep", None),
            P("ep", None),
            P("ep", "tp"),
        ),
        check_vma=False,
    )
```

```python
import functools
import jax
import jax.numpy as jnp
from jax import lax
from jax.experimental import pallas as pl
from jax.experimental.pallas import tpu as pltpu
from jax.sharding import PartitionSpec as P

MESH = pl.DeviceIdType.MESH
CHUNKS = 8
DIRECT = 5


def dispatch_kernel(n_ep, mine_ref, out_ref, local_sem, send_sem, recv_sem, fwd_send, fwd_recv, z_send, z_recv):
    me = lax.axis_index("ep")
    t = lax.axis_index("tp")
    core = lax.rem(t, 2)
    partner = t + 1 - 2 * core
    side_z = lax.rem(t // 2, 2)
    across = t + 2 - 4 * side_z
    width = mine_ref.shape[2] // CHUNKS
    barrier = pltpu.get_barrier_semaphore()
    for d in range(1, n_ep):
        pl.semaphore_signal(
            barrier, inc=1, device_id={"ep": lax.rem(me + d, n_ep)}, device_id_type=MESH
        )
    pl.semaphore_signal(barrier, inc=1, device_id={"tp": partner}, device_id_type=MESH)
    pl.semaphore_signal(barrier, inc=1, device_id={"tp": across}, device_id_type=MESH)
    pl.semaphore_wait(barrier, n_ep + 1)

    def cols(c):
        j, side = (c, side_z) if c < DIRECT else (c - DIRECT, 1 - side_z)
        at = j + side * (CHUNKS - 1 - 2 * j)
        return pl.ds(pl.multiple_of(at * width, 128), width)

    def to_peer(d, c):
        dst = lax.rem(me + d, n_ep)
        return pltpu.make_async_remote_copy(
            src_ref=mine_ref.at[dst, :, cols(c)],
            dst_ref=out_ref.at[core, me, :, cols(c)],
            send_sem=send_sem.at[d, c],
            recv_sem=recv_sem.at[d, c],
            device_id={"ep": dst},
            device_id_type=MESH,
        )

    def from_peer(d, c):
        src = lax.rem(me - d + n_ep, n_ep)
        return pltpu.make_async_remote_copy(
            src_ref=mine_ref.at[me, :, cols(c)],
            dst_ref=out_ref.at[core, src, :, cols(c)],
            send_sem=send_sem.at[d, c],
            recv_sem=recv_sem.at[d, c],
            device_id={"ep": src},
            device_id_type=MESH,
        )

    def forward(d, c, side):
        src = lax.rem(me - d + n_ep, n_ep)
        source = mine_ref.at[me, :, cols(c)] if d == 0 else out_ref.at[side, src, :, cols(c)]
        return pltpu.make_async_remote_copy(
            src_ref=source,
            dst_ref=out_ref.at[side, src, :, cols(c)],
            send_sem=fwd_send.at[d, c],
            recv_sem=fwd_recv.at[d, c],
            device_id={"tp": partner},
            device_id_type=MESH,
        )

    def swap(d, c, arriving):
        src = lax.rem(me - d + n_ep, n_ep)
        ref = out_ref.at[core, src, :, cols(c + DIRECT if arriving else c)]
        return pltpu.make_async_remote_copy(
            src_ref=ref,
            dst_ref=ref,
            send_sem=z_send.at[d, c],
            recv_sem=z_recv.at[d, c],
            device_id={"tp": across},
            device_id_type=MESH,
        )

    order = sorted(range(1, n_ep), key=lambda d: abs(d - n_ep // 2))
    extra = CHUNKS - DIRECT
    for c in range(DIRECT):
        for d in order:
            to_peer(d, c).start()
    keep = pltpu.make_async_copy(mine_ref.at[me], out_ref.at[core, me], local_sem)
    keep.start()
    for c in range(CHUNKS):
        forward(0, c, core).start()
    lag = DIRECT - extra
    for c in range(DIRECT):
        for d in order:
            from_peer(d, c).wait_recv()
            if c < extra:
                swap(d, c, False).start()
            forward(d, c, core).start()
        if c >= lag:
            for d in order:
                swap(d, c - lag, True).wait_recv()
                forward(d, c - lag + DIRECT, core).start()
    keep.wait()
    for c in range(DIRECT):
        for d in order:
            to_peer(d, c).wait_send()
    for c in range(extra):
        for d in order:
            swap(d, c, False).wait_send()
    for d in range(n_ep):
        for c in range(CHUNKS):
            forward(d, c, core).wait_send()
            forward(d, c, 1 - core).wait_recv()


def dispatch(mine, n_ep):
    return pl.pallas_call(
        functools.partial(dispatch_kernel, n_ep),
        out_shape=jax.ShapeDtypeStruct((2,) + mine.shape, mine.dtype),
        in_specs=[pl.BlockSpec(memory_space=pltpu.VMEM)],
        out_specs=pl.BlockSpec(memory_space=pl.ANY),
        scratch_shapes=[
            pltpu.SemaphoreType.DMA,
            pltpu.SemaphoreType.DMA((n_ep, CHUNKS)),
            pltpu.SemaphoreType.DMA((n_ep, CHUNKS)),
            pltpu.SemaphoreType.DMA((n_ep, CHUNKS)),
            pltpu.SemaphoreType.DMA((n_ep, CHUNKS)),
            pltpu.SemaphoreType.DMA((n_ep, CHUNKS)),
            pltpu.SemaphoreType.DMA((n_ep, CHUNKS)),
        ],
        compiler_params=pltpu.CompilerParams(collective_id=0, has_side_effects=True),
        name="dispatch",
    )(mine)


def sums_kernel(n_ep, n_tp, part_ref, norm_ref, score_ref, slots, total, send_sem, recv_sem, s_send, s_recv):
    me = lax.axis_index("ep")
    t = lax.axis_index("tp")
    barrier = pltpu.get_barrier_semaphore()
    for d in range(1, n_tp):
        pl.semaphore_signal(
            barrier, inc=1, device_id={"tp": lax.rem(t + d, n_tp)}, device_id_type=MESH
        )
    for d in range(1, n_ep):
        pl.semaphore_signal(
            barrier, inc=1, device_id={"ep": lax.rem(me + d, n_ep)}, device_id_type=MESH
        )
    pl.semaphore_wait(barrier, n_tp - 1 + n_ep - 1)

    def part_to(d):
        return pltpu.make_async_remote_copy(
            src_ref=part_ref,
            dst_ref=slots.at[t],
            send_sem=send_sem.at[d],
            recv_sem=recv_sem.at[d],
            device_id={"tp": lax.rem(t + d, n_tp)},
            device_id_type=MESH,
        )

    def part_from(d):
        src = lax.rem(t - d + n_tp, n_tp)
        return pltpu.make_async_remote_copy(
            src_ref=part_ref,
            dst_ref=slots.at[src],
            send_sem=send_sem.at[d],
            recv_sem=recv_sem.at[d],
            device_id={"tp": src},
            device_id_type=MESH,
        )

    for d in range(1, n_tp):
        part_to(d).start()
    slots[t] = part_ref[...]
    for d in range(1, n_tp):
        part_from(d).wait_recv()
    acc = slots[0]
    for i in range(1, n_tp):
        acc = acc + slots[i]
    total[...] = acc
    rows = 8 * n_ep

    def score_to(d):
        dst = lax.rem(me + d, n_ep)
        return pltpu.make_async_remote_copy(
            src_ref=total.at[pl.ds(pl.multiple_of(dst * 8, 8), 8)],
            dst_ref=score_ref.at[me],
            send_sem=s_send.at[d],
            recv_sem=s_recv.at[d],
            device_id={"ep": dst},
            device_id_type=MESH,
        )

    def score_from(d):
        src = lax.rem(me - d + n_ep, n_ep)
        return pltpu.make_async_remote_copy(
            src_ref=total.at[pl.ds(0, 8)],
            dst_ref=score_ref.at[src],
            send_sem=s_send.at[d],
            recv_sem=s_recv.at[d],
            device_id={"ep": src},
            device_id_type=MESH,
        )

    norm_ref[...] = acc[rows:]
    for d in range(1, n_tp):
        part_to(d).wait_send()
    for d in range(1, n_ep):
        score_to(d).start()
    score_ref[me] = total[pl.ds(pl.multiple_of(me * 8, 8), 8)]
    for d in range(1, n_ep):
        score_from(d).wait_recv()
    for d in range(1, n_ep):
        score_to(d).wait_send()


def small_sums(scores, norms, n_ep, n_tp):
    cap = scores.shape[1]
    width = norms.shape[1]
    padded = jnp.pad(scores, ((0, 0), (0, 1024 - cap))).reshape(n_ep * 8, 128)
    part = jnp.concatenate([padded, norms.reshape(2 * width // 128, 128)], axis=0)
    norm_out, score_out = pl.pallas_call(
        functools.partial(sums_kernel, n_ep, n_tp),
        out_shape=(
            jax.ShapeDtypeStruct((2 * width // 128, 128), jnp.float32),
            jax.ShapeDtypeStruct((n_ep, 8, 128), jnp.float32),
        ),
        in_specs=[pl.BlockSpec(memory_space=pltpu.VMEM)],
        out_specs=(
            pl.BlockSpec(memory_space=pltpu.VMEM),
            pl.BlockSpec(memory_space=pltpu.VMEM),
        ),
        scratch_shapes=[
            pltpu.VMEM((n_tp,) + part.shape, jnp.float32),
            pltpu.VMEM(part.shape, jnp.float32),
            pltpu.SemaphoreType.DMA((n_tp,)),
            pltpu.SemaphoreType.DMA((n_tp,)),
            pltpu.SemaphoreType.DMA((n_ep,)),
            pltpu.SemaphoreType.DMA((n_ep,)),
        ],
        compiler_params=pltpu.CompilerParams(collective_id=1, has_side_effects=True),
        cost_estimate=pl.CostEstimate(flops=0, bytes_accessed=20_000_000, transcendentals=0),
        name="small_sums",
    )(part)
    return score_out.reshape(n_ep, 1024)[:, :cap], norm_out.reshape(2, width)


def finish_kernel(
    n_ep, n_tp, both_ref, gate_ref, up_ref, hid_ref, part_ref, score_ref, pick_ref,
    out_ref, gate_out, up_out, down_out, norm_ref, down_norm_ref, score_out,
    rows_in, rows_scaled, gate_v, up_v, hid_v, gate_g, up_g, down_g, norm_part,
    s_slots, s_total, n_slots, bufs, accs, returned,
    load_sem, store_sem, rs_send, rs_recv, ep_send, ep_recv, ag_send, ag_recv,
    sc_send, sc_recv, sx_send, sx_recv, nm_send, nm_recv,
):
    me = lax.axis_index("ep")
    t = lax.axis_index("tp")
    cap, width = part_ref.shape[1], part_ref.shape[2]
    ff = gate_v.shape[1]
    tok = out_ref.shape[0]
    levels = len(bufs)
    bits = [lax.rem(t // (1 << s), 2) for s in range(levels)]
    peers = [t + (1 - 2 * bits[s]) * (1 << s) for s in range(levels)]

    def remote(src, dst, send, recv, device):
        return pltpu.make_async_remote_copy(
            src_ref=src, dst_ref=dst, send_sem=send, recv_sem=recv,
            device_id=device, device_id_type=MESH,
        )

    loads = []
    for b in range(n_ep):
        loads.append(pltpu.make_async_copy(
            both_ref.at[0, b], rows_in.at[pl.ds(b * cap, cap)], load_sem.at[len(loads)]))
        loads.append(pltpu.make_async_copy(
            both_ref.at[1, b], rows_scaled.at[pl.ds(b * cap, cap)], load_sem.at[len(loads)]))
    for src, dst in ((gate_ref, gate_v), (up_ref, up_v), (hid_ref, hid_v)):
        loads.append(pltpu.make_async_copy(src, dst, load_sem.at[len(loads)]))

    barrier = pltpu.get_barrier_semaphore()
    for d in range(1, n_tp):
        pl.semaphore_signal(
            barrier, inc=1, device_id={"tp": lax.rem(t + d, n_tp)}, device_id_type=MESH
        )
    for d in range(1, n_ep):
        pl.semaphore_signal(
            barrier, inc=1, device_id={"ep": lax.rem(me + d, n_ep)}, device_id_type=MESH
        )
    pl.semaphore_wait(barrier, n_tp - 1 + n_ep - 1)

    order = sorted(range(1, n_ep), key=lambda d: abs(d - n_ep // 2)) + [0]

    def block(i):
        return lax.rem(me + order[i], n_ep)

    def halves(s):
        w = width >> (s + 1)
        keep = pl.ds(pl.multiple_of(bits[s] * w, 128), w)
        give = pl.ds(pl.multiple_of((1 - bits[s]) * w, 128), w)
        return keep, give

    def exchange(s, i):
        _, give = halves(s)
        src = part_ref.at[block(i), :, give] if s == 0 else accs[s - 1].at[i, :, give]
        return remote(src, bufs[s].at[i], rs_send.at[s, i], rs_recv.at[s, i], {"tp": peers[s]})

    def to_owner(i):
        d = order[i]
        return remote(
            accs[levels - 1].at[i],
            returned.at[pl.ds(pl.multiple_of(me * cap, 16), cap)],
            ep_send.at[d], ep_recv.at[d], {"ep": block(i)},
        )

    def from_owner(d):
        src = lax.rem(me - d + n_ep, n_ep)
        return remote(
            accs[levels - 1].at[0],
            returned.at[pl.ds(pl.multiple_of(src * cap, 16), cap)],
            ep_send.at[d], ep_recv.at[d], {"ep": src},
        )

    def score_to(d):
        return remote(score_ref, s_slots.at[t], sc_send.at[d], sc_recv.at[d],
                      {"tp": lax.rem(t + d, n_tp)})

    def score_from(d):
        src = lax.rem(t - d + n_tp, n_tp)
        return remote(score_ref, s_slots.at[src], sc_send.at[d], sc_recv.at[d], {"tp": src})

    def norm_to(d):
        return remote(norm_part, n_slots.at[t], nm_send.at[d], nm_recv.at[d],
                      {"tp": lax.rem(t + d, n_tp)})

    def norm_from(d):
        src = lax.rem(t - d + n_tp, n_tp)
        return remote(norm_part, n_slots.at[src], nm_send.at[d], nm_recv.at[d], {"tp": src})

    def score_back(d):
        dst = lax.rem(me + d, n_ep)
        return remote(s_total.at[pl.ds(pl.multiple_of(dst * 8, 8), 8)], score_out.at[me],
                      sx_send.at[d], sx_recv.at[d], {"ep": dst})

    def score_arrive(d):
        src = lax.rem(me - d + n_ep, n_ep)
        return remote(s_total.at[pl.ds(0, 8)], score_out.at[src],
                      sx_send.at[d], sx_recv.at[d], {"ep": src})

    for i in range(n_ep):
        exchange(0, i).start()
    for d in range(1, n_tp):
        score_to(d).start()
    for copy in loads:
        copy.start()
    s_slots[t] = score_ref[...]

    rows = (((0,), (0,)), ((), ()))
    step = 256
    half = width // step // 2

    def fold(sq):
        parts = [sq[:, j * 128:(j + 1) * 128] for j in range(sq.shape[1] // 128)]
        return functools.reduce(jnp.add, parts)

    def line(x):
        return jnp.sum(jnp.transpose(x), axis=0, keepdims=True)

    def gate_up(first):
        def body(j, carry):
            at = pl.ds(pl.multiple_of(j * step, step), step)
            lhs = rows_in[:, at]
            for n, (rhs, out) in enumerate(((gate_v, gate_g), (up_v, up_g))):
                total = lax.dot_general(lhs, rhs[...], rows, preferred_element_type=jnp.float32)
                out[at, :] = total.astype(jnp.bfloat16)
                sq = fold(total * total)
                for h in range(step // 128):
                    norm_part[n, pl.ds(j * (step // 128) + h, 1), :] = line(
                        sq[h * 128:(h + 1) * 128]
                    ) / (ff * n_tp)
            return carry
        lax.fori_loop(first, first + half, body, 0)

    def down():
        def body(j, carry):
            at = pl.ds(pl.multiple_of(j * step, step), step)
            lhs = hid_v[:, at]
            sq = None
            for c in range(0, width, 512):
                total = lax.dot_general(
                    lhs, rows_scaled[:, c:c + 512], rows, preferred_element_type=jnp.float32
                )
                down_g[at, c:c + 512] = total.astype(jnp.bfloat16)
                more = fold(total * total)
                sq = more if sq is None else sq + more
            for h in range(step // 128):
                down_norm_ref[pl.ds(j * (step // 128) + h, 1), :] = line(
                    sq[h * 128:(h + 1) * 128]
                ) / width
            return carry
        lax.fori_loop(0, ff // step, body, 0)

    stores = [
        pltpu.make_async_copy(a, b, store_sem.at[n])
        for n, (a, b) in enumerate(((gate_g, gate_out), (up_g, up_out), (down_g, down_out)))
    ]

    def work_first():
        for copy in loads:
            copy.wait()
        gate_up(0)

    def work_second():
        gate_up(half)
        for d in range(1, n_tp):
            norm_to(d).start()
        n_slots[t] = norm_part[...]
        stores[0].start()
        stores[1].start()

    def work_third():
        for d in range(1, n_tp):
            score_from(d).wait_recv()
        acc = s_slots[0]
        for i in range(1, n_tp):
            acc = acc + s_slots[i]
        s_total[...] = acc
        down()
        stores[2].start()
        for d in range(1, n_ep):
            score_back(d).start()
        score_out[me] = s_total[pl.ds(pl.multiple_of(me * 8, 8), 8)]

    work = [work_first, work_second, work_third]
    for tick in range(max(n_ep + levels - 1, len(work))):
        for i in range(n_ep):
            s = tick - i
            if not 0 <= s < levels:
                continue
            exchange(s, i).wait_recv()
            keep, _ = halves(s)
            own = part_ref[block(i), :, keep] if s == 0 else accs[s - 1][i, :, keep]
            total = own.astype(jnp.float32) + bufs[s][i].astype(jnp.float32)
            accs[s][i] = total.astype(jnp.bfloat16)
            if s + 1 < levels:
                exchange(s + 1, i).start()
            elif order[i]:
                to_owner(i).start()
            else:
                returned[pl.ds(pl.multiple_of(me * cap, 16), cap), :] = total.astype(jnp.bfloat16)
        if tick < len(work):
            work[tick]()

    for d in range(1, n_ep):
        from_owner(d).wait_recv()
    share = width >> levels
    base = [None] * (levels + 1)
    base[0] = 0
    for s in range(levels):
        base[s + 1] = base[s] + bits[s] * (width >> (s + 1))
    pieces = 2
    piece = tok // pieces

    def spread(s, p):
        w = width >> (s + 1)
        at = pl.ds(pl.multiple_of(base[s + 1], 128), w)
        ref = out_ref.at[pl.ds(p * piece, piece), at]
        return remote(ref, ref, ag_send.at[s, p], ag_recv.at[s, p], {"tp": peers[s]})

    def arrived(s, p):
        w = width >> (s + 1)
        at = pl.ds(pl.multiple_of(base[s] + (1 - bits[s]) * w, 128), w)
        ref = out_ref.at[pl.ds(p * piece, piece), at]
        return remote(ref, ref, ag_send.at[s, p], ag_recv.at[s, p], {"tp": peers[s]})

    for p in range(pieces):
        grad = jnp.dot(
            pick_ref[p * piece:(p + 1) * piece, :], returned[...],
            preferred_element_type=jnp.float32,
        )
        out_ref[p * piece:(p + 1) * piece, pl.ds(pl.multiple_of(base[levels], 128), share)] = (
            grad.astype(jnp.bfloat16)
        )
        spread(levels - 1, p).start()
    for d in range(1, n_tp):
        norm_from(d).wait_recv()
    acc = n_slots[0]
    for i in range(1, n_tp):
        acc = acc + n_slots[i]
    norm_ref[...] = acc
    for s in reversed(range(levels)):
        for p in range(pieces):
            arrived(s, p).wait_recv()
            if s:
                spread(s - 1, p).start()

    for d in range(1, n_ep):
        score_arrive(d).wait_recv()
        score_back(d).wait_send()
    for i in range(n_ep):
        for s in range(levels):
            exchange(s, i).wait_send()
        if order[i]:
            to_owner(i).wait_send()
    for d in range(1, n_tp):
        score_to(d).wait_send()
        norm_to(d).wait_send()
    for s in range(levels):
        for p in range(pieces):
            spread(s, p).wait_send()
    for copy in stores:
        copy.wait()


def finish(both, gate_pre, up_pre, hidden, part, score_part, pick_t, n_ep, n_tp):
    cap, width = part.shape[1:]
    rows, ff = gate_pre.shape
    tok = pick_t.shape[0]
    levels = n_tp.bit_length() - 1
    scores = jnp.pad(score_part, ((0, 0), (0, 1024 - cap))).reshape(n_ep * 8, 128)
    bf, f32 = jnp.bfloat16, jnp.float32
    vmem = pl.BlockSpec(memory_space=pltpu.VMEM)
    hbm = pl.BlockSpec(memory_space=pl.ANY)
    dma = pltpu.SemaphoreType.DMA
    stages = [pltpu.VMEM((n_ep, cap, width >> (s + 1)), bf) for s in range(levels)]
    outs = pl.pallas_call(
        functools.partial(finish_kernel, n_ep, n_tp),
        out_shape=(
            jax.ShapeDtypeStruct((tok, width), bf),
            jax.ShapeDtypeStruct((width, ff), bf),
            jax.ShapeDtypeStruct((width, ff), bf),
            jax.ShapeDtypeStruct((ff, width), bf),
            jax.ShapeDtypeStruct((2, width // 128, 128), f32),
            jax.ShapeDtypeStruct((ff // 128, 128), f32),
            jax.ShapeDtypeStruct((n_ep, 8, 128), f32),
        ),
        in_specs=[hbm, hbm, hbm, hbm, vmem, vmem, vmem],
        out_specs=(vmem, hbm, hbm, hbm, vmem, vmem, vmem),
        scratch_shapes=[
            pltpu.VMEM((rows, width), bf),
            pltpu.VMEM((rows, width), bf),
            pltpu.VMEM((rows, ff), bf),
            pltpu.VMEM((rows, ff), bf),
            pltpu.VMEM((rows, ff), bf),
            pltpu.VMEM((width, ff), bf),
            pltpu.VMEM((width, ff), bf),
            pltpu.VMEM((ff, width), bf),
            pltpu.VMEM((2, width // 128, 128), f32),
            pltpu.VMEM((n_tp,) + scores.shape, f32),
            pltpu.VMEM(scores.shape, f32),
            pltpu.VMEM((n_tp, 2, width // 128, 128), f32),
            list(stages),
            list(stages),
            pltpu.VMEM((rows, width >> levels), bf),
            dma((2 * n_ep + 3,)),
            dma((3,)),
            dma((levels, n_ep)),
            dma((levels, n_ep)),
            dma((n_ep,)),
            dma((n_ep,)),
            dma((levels, 2)),
            dma((levels, 2)),
            dma((n_tp,)),
            dma((n_tp,)),
            dma((n_ep,)),
            dma((n_ep,)),
            dma((n_tp,)),
            dma((n_tp,)),
        ],
        compiler_params=pltpu.CompilerParams(
            collective_id=2, has_side_effects=True, vmem_limit_bytes=48 << 20
        ),
        name="finish",
    )(both, gate_pre, up_pre, hidden, part, scores, pick_t)
    token_grad, gate_g, up_g, down_g, norms, down_norms, score_out = outs
    return (
        token_grad, gate_g, up_g, down_g, norms.reshape(2, width),
        down_norms.reshape(ff), score_out.reshape(n_ep, 1024)[:, :cap],
    )


def local(tokens, cotangent, group_prob, expert_prob, routing, gate_weight, up_weight, down_weight):
    tok_count, model_width = tokens.shape
    top_count = routing.shape[1]
    n_ep = lax.axis_size("ep")
    n_tp = lax.axis_size("tp")
    capacity = 3 * tok_count * top_count // (2 * n_ep)
    buffer_rows = n_ep * capacity
    core = lax.rem(lax.axis_index("tp"), 2)
    weight = group_prob[:, None] * expert_prob

    experts = jnp.arange(n_ep, dtype=jnp.int32)[:, None]
    picks = [routing[None, :, k] == experts for k in range(top_count)]
    named = functools.reduce(jnp.logical_or, picks)
    weight_of = sum(jnp.where(picks[k], weight[None, :, k], 0.0) for k in range(top_count))
    earlier = (
        lax.broadcasted_iota(jnp.int32, (tok_count, tok_count), 0)
        < lax.broadcasted_iota(jnp.int32, (tok_count, tok_count), 1)
    ).astype(jnp.bfloat16)
    before = jnp.dot(named.astype(jnp.bfloat16), earlier, preferred_element_type=jnp.float32)
    place = jnp.where(named, before.astype(jnp.int32), -1)
    filled = place[:, None, :] == lax.broadcasted_iota(jnp.int32, (n_ep, capacity, tok_count), 1)
    pick = filled.astype(jnp.bfloat16).reshape(buffer_rows, tok_count)
    slot_weight = jnp.sum(jnp.where(filled, weight_of[:, None, :], 0.0), axis=2).reshape(buffer_rows, 1)

    source = jnp.where(core == 0, tokens, cotangent)
    factor = jnp.where(core == 0, 1.0, slot_weight)
    mine = jnp.dot(pick, source, preferred_element_type=jnp.float32) * factor
    mine = mine.astype(jnp.bfloat16).reshape(n_ep, capacity, model_width)
    both = dispatch(mine, n_ep)
    flat_in = both[0].reshape(buffer_rows, model_width)
    flat_scaled = both[1].reshape(buffer_rows, model_width)

    w_gate = gate_weight[0]
    w_up = up_weight[0]
    w_down = down_weight[0]
    hidden_total = gate_weight.shape[2] * n_tp
    contract_last = (((1,), (1,)), ((), ()))
    contract_rows = (((0,), (0,)), ((), ()))
    pre_gate = jnp.dot(flat_in, w_gate, preferred_element_type=jnp.float32)
    pre_up = jnp.dot(flat_in, w_up, preferred_element_type=jnp.float32)
    sigma = jax.nn.sigmoid(pre_gate)
    activated = pre_gate * sigma
    derivative = sigma * (1.0 + pre_gate * (1.0 - sigma))
    hidden = (activated * pre_up).astype(jnp.bfloat16)
    hidden_grad = lax.dot_general(
        flat_scaled, w_down, contract_last, preferred_element_type=jnp.float32
    )
    score_part = jnp.sum(hidden.astype(jnp.float32) * hidden_grad, axis=1).reshape(n_ep, capacity)
    gate_pre = (hidden_grad * pre_up * derivative).astype(jnp.bfloat16)
    up_pre = (hidden_grad * activated).astype(jnp.bfloat16)
    input_part = lax.dot_general(
        gate_pre, w_gate, contract_last, preferred_element_type=jnp.float32
    )
    input_part = input_part + lax.dot_general(
        up_pre, w_up, contract_last, preferred_element_type=jnp.float32
    )
    input_part = input_part.astype(jnp.bfloat16).reshape(n_ep, capacity, model_width)
    if n_tp & (n_tp - 1) == 0 and model_width // n_tp % 128 == 0:
        pick_t = pick.T
        token_grad, gate_grad, up_grad, down_grad, row_norms, down_norms, scores = finish(
            both, gate_pre, up_pre, hidden, input_part, score_part, pick_t, n_ep, n_tp
        )
    else:
        share = lax.psum_scatter(input_part, "tp", scatter_dimension=2, tiled=True)

        down_sum = lax.dot_general(
            hidden, flat_scaled, contract_rows, preferred_element_type=jnp.float32
        )
        gate_sum = lax.dot_general(flat_in, gate_pre, contract_rows, preferred_element_type=jnp.float32)
        up_sum = lax.dot_general(flat_in, up_pre, contract_rows, preferred_element_type=jnp.float32)
        norm_part = (
            jnp.stack([jnp.sum(gate_sum * gate_sum, axis=1), jnp.sum(up_sum * up_sum, axis=1)])
            / hidden_total
        )
        down_norms = jnp.sum(down_sum * down_sum, axis=1) / model_width
        scores, row_norms = small_sums(score_part, norm_part, n_ep, n_tp)

        share, scores, row_norms, down_norms = lax.optimization_barrier(
            (share, scores, row_norms, down_norms)
        )
        returned = lax.all_to_all(share, "ep", split_axis=0, concat_axis=0, tiled=True)
        returned = returned.reshape(buffer_rows, -1)
        token_share = lax.dot_general(pick, returned, contract_rows, preferred_element_type=jnp.float32)
        token_grad = lax.all_gather(token_share.astype(jnp.bfloat16), "tp", axis=1, tiled=True)
        gate_grad, up_grad, down_grad = (
            x.astype(jnp.bfloat16) for x in (gate_sum, up_sum, down_sum)
        )

    score_of = jnp.sum(jnp.where(filled, scores[:, :, None], 0.0), axis=1)
    slot_score = jnp.stack(
        [jnp.sum(jnp.where(p, score_of, 0.0), axis=0) for p in picks], axis=1
    ) / weight
    expert_prob_grad = group_prob[:, None] * slot_score
    group_prob_grad = jnp.sum(expert_prob * slot_score, axis=1)
    return (
        token_grad,
        group_prob_grad,
        expert_prob_grad,
        gate_grad[None],
        up_grad[None],
        down_grad[None],
        row_norms[0][None],
        row_norms[1][None],
        down_norms[None],
    )


def solution(mesh):
    return jax.shard_map(
        local,
        mesh=mesh,
        in_specs=(
            P("ep", None),
            P("ep", None),
            P("ep"),
            P("ep", None),
            P("ep", None),
            P("ep", None, "tp"),
            P("ep", None, "tp"),
            P("ep", "tp", None),
        ),
        out_specs=(
            P("ep", None),
            P("ep"),
            P("ep", None),
            P("ep", None, "tp"),
            P("ep", None, "tp"),
            P("ep", "tp", None),
            P("ep", None),
            P("ep", None),
            P("ep", "tp"),
        ),
        check_vma=False,
    )
```
